32 devices in a mesh: sp: 8 (over z, core), tp: 4 (over y, x).
Axes of the slice: x: 2, y: 2, z: 4, core: 2. Of those that a mesh axis runs over, the one named last changes fastest.
Arguments:
- cotangent: bfloat16 [1024, 2048], P('sp'), may hold values from -6 to 6
- moe_input: bfloat16 [1024, 2048], P('sp'), may hold values from -6 to 6
- expert_ids: int32 [1024, 2], P('sp'), may hold values from 0 to 7, all different within a row; in each aligned block of 128 rows (0 to 127, 128 to 255, ...) at most 48 rows name the same one
- group_weight: float32 [1024], P('sp'), may hold values from 0.3 to 1
- expert_weight: float32 [1024, 2], P('sp'), may hold values from 0.1 to 0.9
- mixer_out: bfloat16 [1024, 512], P('sp', 'tp'), may hold values from -6 to 6
- queries: bfloat16 [256, 1024], P('tp', 'sp'), may hold values from -6 to 6
- key_vectors: bfloat16 [256, 1024], P('tp', 'sp'), may hold values from -6 to 6
- value_vectors: bfloat16 [512, 1024], P('tp', 'sp'), may hold values from -6 to 6
- decay_rates: float32 [4, 1024], P('tp', 'sp'), may hold values from 0 to 1, as said below
- proj_weight: bfloat16 [2048, 512], P(None, 'tp'), may hold values from -0.25 to 0.25
- gate_weight: bfloat16 [8, 2048, 2048], P('sp', None, 'tp'), may hold values from -0.125 to 0.125
- up_weight: bfloat16 [8, 2048, 2048], P('sp', None, 'tp'), may hold values from -0.125 to 0.125
- down_weight: bfloat16 [8, 2048, 2048], P('sp', 'tp'), may hold values from -0.125 to 0.125
Outputs:
- grad_gate: bfloat16 [8, 2048, 2048], P('sp', None, 'tp')
- grad_up: bfloat16 [8, 2048, 2048], P('sp', None, 'tp')
- grad_down: bfloat16 [8, 2048, 2048], P('sp', 'tp')
- grad_proj: float32 [2048, 512], P('sp', 'tp')
- grad_queries: float32 [256, 1024], P('tp', 'sp')
- grad_keys: float32 [256, 1024], P('tp', 'sp')
- grad_values: float32 [512, 1024], P('tp', 'sp')
The draws below stay inside these ranges and needn't reach their ends.
Inputs may be any that keep to these rules, and one draw needn't show every extreme that they name: `expert_ids`: in the rows of one device no expert is named by more than 48 entries, a bound that some block reaches; the 2 experts of a row differ. `decay_rates`: Positive.
All inputs are finite; a program needn't handle non-finite values.
Results may differ from the reference program's by a relative error of at most 0.0058.
Values may be sent and summed in bfloat16 or wider, within the bound.
A program may use at most 64 MiB of HBM per device.

```python
import math
from functools import partial
import jax
import jax.numpy as jnp
import numpy as np
from jax import lax

D = 2048
KD = 64
VD = 128
RETENTION_HEADS = 4
FF = 2048
EXPERTS = 8
TOP = 2
TOK_DEV = 128
SEQUENCE_TOKENS = 1024
CAP = 48
N_SP = 8


def draw_decay_rates(key, part):
    random_subkeys = jax.random.split(key, 6)
    fast_share = 0.5
    fast_heads = jax.random.uniform(random_subkeys[0], (RETENTION_HEADS, 1)) < fast_share
    block_count = SEQUENCE_TOKENS // TOK_DEV
    block_multiplier = jax.random.uniform(random_subkeys[1], (RETENTION_HEADS, block_count, 1), minval=0.5, maxval=1.5)
    block_multiplier = jnp.broadcast_to(block_multiplier, (RETENTION_HEADS, block_count, TOK_DEV)).reshape(RETENTION_HEADS, SEQUENCE_TOKENS)
    jaggedness = jnp.exp(jax.random.uniform(random_subkeys[2], (RETENTION_HEADS, SEQUENCE_TOKENS), minval=math.log(0.7), maxval=math.log(1.4)))
    fast_rate = jnp.exp(jax.random.uniform(random_subkeys[3], (RETENTION_HEADS, 1), minval=math.log(1.0 / 40.0), maxval=math.log(1.0 / 15.0)))
    baseline_rate = jnp.where(fast_heads, fast_rate, 0.8 / SEQUENCE_TOKENS)
    spike_position = jax.random.randint(random_subkeys[4], (RETENTION_HEADS, 2, 1), 0, SEQUENCE_TOKENS)
    spike_penalty = jax.random.uniform(random_subkeys[5], (RETENTION_HEADS, 2, 1), minval=0.2, maxval=0.4)
    token_positions = jnp.arange(SEQUENCE_TOKENS, dtype=jnp.int32)[None, None, :]
    spike_events = jnp.sum(jnp.where(token_positions == spike_position, -jnp.log(1.0 - spike_penalty), 0.0), axis=1)
    return (baseline_rate * block_multiplier * jaggedness + spike_events).astype(jnp.float32)


def with_spikes(array, rng, source, target, blocks, factor):
    owner, partner = [(jnp.arange(array.shape[dim]) // (array.shape[dim] // blocks)).reshape([-1 if axis == dim else 1 for axis in range(array.ndim)]) for dim in (source, target)]
    chosen = jax.random.permutation(rng, blocks)[partner]
    strong = (owner == chosen) | (owner == (partner + blocks // 2) % blocks)
    return jnp.where(strong, factor * array, array)


def level_of(rng, shape, pieces, low, high):
    def one(dim, blocks):
        heights = jax.random.uniform(jax.random.fold_in(jax.random.fold_in(rng, 6), dim), (blocks,), jnp.float32, low / len(pieces), high / len(pieces))
        return jnp.repeat(jnp.exp(heights), shape[dim] // blocks).reshape((-1,) + (1,) * (len(shape) - dim - 1))

    loudness = one(*pieces[0])
    for cut in pieces[1:]:
        loudness = loudness * one(*cut)
    return loudness


def shared_out(key, own, number, rows, count, top, most, skew):
    order = jax.random.permutation(key, count)
    packed, common = shares(count, rows * top, most, skew, True), shares(count, rows * top, most, skew, False)
    places = jnp.arange(count)

    def named(tallies, rotation):
        used = int((tallies > 0).sum())
        fixed = max(1, used // 4)
        moved = fixed + (places - fixed + rotation * (used - fixed)) % max(1, count - fixed)
        return jnp.zeros((count,), jnp.int32).at[order[jnp.where(places < fixed, places, moved)]].set(jnp.asarray(tallies, jnp.int32))

    tallies = jnp.where(number % 4 == 0, named(packed, number // 4), named(common, number - number // 4 - 1))
    mixed = jax.random.permutation(jax.random.fold_in(own, 3), count)
    source_of, taker = mixed[0:count // 2 * 2:2], mixed[1:count // 2 * 2:2]
    room = jnp.minimum(tallies[source_of] - 1, most - tallies[taker]) // 2
    room = jnp.where((source_of == order[0]) | (taker == order[0]) | (tallies[taker] == 0), 0, jnp.maximum(room, 0))
    moved = jax.random.randint(jax.random.fold_in(own, 4), (count // 2,), 0, 1 << 20) % (room + 1)
    tallies = tallies.at[source_of].add(-moved).at[taker].add(moved)
    members = jnp.searchsorted(jnp.cumsum(tallies), jnp.arange(rows * top), side="right").astype(jnp.int32)
    table = members.reshape(top, rows).T
    table = table[jax.random.permutation(jax.random.fold_in(own, 1), rows)]
    rotation = jax.random.randint(jax.random.fold_in(own, 2), (rows, 1), 0, top)
    return jnp.take_along_axis(table, (jnp.arange(top)[None, :] + rotation) % top, axis=1)


def shares(count, total, bound, slope, full):
    loads = [(1 << 20) // math.isqrt(grade ** slope) + 1 for grade in range(1, count + 1)]
    largest = bound if full else min(bound, max(-(-total // count), total * loads[0] // sum(loads)))
    least = 1 if total - largest >= count - 1 else 0
    holding, spare = [largest] + [least] * (count - 1), total - largest - least * (count - 1)
    while spare > 0:
        free = [i for i in range(1, count) if holding[i] < largest] or [i for i in range(1, count) if holding[i] < bound]
        pool, remaining = sum([loads[i] for i in free]), spare
        for i in free:
            addition = min(bound - holding[i], max(1, remaining * loads[i] // pool), spare)
            holding[i] = holding[i] + addition
            spare = spare - addition
    return np.array(holding)


def bell_draw(key, shape, width, limit, cuts=(), held_as=jnp.bfloat16):
    loudness = level_of(key, shape, cuts, -0.22, 0.18) if cuts else 1.0
    values = jax.random.normal(key, shape, jnp.float32) * width * loudness
    return jnp.minimum(jnp.maximum(values, -limit), limit).astype(held_as)


def noise_with(key, dims, deviation, reach, pieces, heavy, kind=jnp.bfloat16):
    array = deviation * jax.random.normal(key, dims, jnp.float32)
    if pieces:
        array = array * level_of(key, dims, pieces, -0.22, 0.18)
    return jnp.clip(with_spikes(array, jax.random.fold_in(key, 3), *heavy), -reach, reach).astype(kind)


def setup_inputs(seed: int = 0) -> dict:
    splits = jax.random.split(jax.random.key(seed), 15)
    cotangent = noise_with(splits[0], (SEQUENCE_TOKENS, D), 1.0, 6.0, ((0, 8),), (0, 1, 8, 2.0))
    moe_input = bell_draw(splits[1], (SEQUENCE_TOKENS, D), 1.0, 6.0, ((0, 8),))
    expert_ids_keys = jax.random.split(jax.random.fold_in(splits[2], 1), SEQUENCE_TOKENS // TOK_DEV)
    expert_ids_turns = jax.random.permutation(jax.random.fold_in(splits[2], 3), SEQUENCE_TOKENS // TOK_DEV)
    expert_ids = jax.vmap(lambda own, number: shared_out(jax.random.fold_in(splits[2], 2), own, number, TOK_DEV, EXPERTS, TOP, CAP, 1))(expert_ids_keys, expert_ids_turns).reshape((SEQUENCE_TOKENS, TOP))
    group_weight = jnp.clip(0.3 + 0.7 * jax.random.uniform(splits[3], (SEQUENCE_TOKENS,), jnp.float32) ** level_of(splits[3], (SEQUENCE_TOKENS,), ((0, 8),), -0.2, 0.2), 0.3, 1.0)
    expert_weight = jnp.clip(0.1 + 0.79999997 * jax.random.uniform(splits[4], (SEQUENCE_TOKENS, TOP), jnp.float32) ** level_of(splits[4], (SEQUENCE_TOKENS, TOP), ((0, 8),), -0.2, 0.2), 0.1, 0.9)
    mixer_out = bell_draw(splits[5], (SEQUENCE_TOKENS, RETENTION_HEADS * VD), 1.0, 6.0, ((0, 8), (1, 4)))
    queries = bell_draw(splits[6], (RETENTION_HEADS * KD, SEQUENCE_TOKENS), 1.0, 6.0, ((0, 4), (1, 8)))
    key_vectors = bell_draw(splits[7], (RETENTION_HEADS * KD, SEQUENCE_TOKENS), 1.0, 6.0, ((0, 4), (1, 8)))
    value_vectors = bell_draw(splits[8], (RETENTION_HEADS * VD, SEQUENCE_TOKENS), 1.0, 6.0, ((0, 4), (1, 8)))
    decay_rates = draw_decay_rates(jax.random.fold_in(splits[14], 71), 0)
    proj_weight = bell_draw(splits[10], (D, RETENTION_HEADS * VD), (RETENTION_HEADS * VD) ** -0.5, 0.25, ((1, 4),))
    gate_weight = bell_draw(splits[11], (EXPERTS, D, FF), D ** -0.5, 0.125, ((0, 8), (2, 4)))
    up_weight = bell_draw(splits[12], (EXPERTS, D, FF), D ** -0.5, 0.125, ((0, 8), (2, 4)))
    down_weight = bell_draw(splits[13], (EXPERTS, FF, D), FF ** -0.5, 0.125, ((0, 8), (1, 4)))
    return dict(cotangent=cotangent, moe_input=moe_input, expert_ids=expert_ids, group_weight=group_weight, expert_weight=expert_weight, mixer_out=mixer_out, queries=queries, key_vectors=key_vectors, value_vectors=value_vectors, decay_rates=decay_rates, proj_weight=proj_weight, gate_weight=gate_weight, up_weight=up_weight, down_weight=down_weight)


def slot_table(block_ids, experts_all, capacity):
    flat_ids = block_ids.reshape(-1).astype(jnp.int32)
    expert_range = jnp.arange(experts_all, dtype=jnp.int32)
    onehot = (flat_ids[:, None] == expert_range[None, :]).astype(jnp.int32)
    before = jnp.cumsum(onehot, axis=0) - onehot
    rank_in = jnp.sum(before * onehot, axis=1)
    slot_ids = flat_ids * capacity + rank_in
    slot_range = jnp.arange(experts_all * capacity, dtype=jnp.int32)
    entry_numbers = jnp.arange(1, flat_ids.shape[0] + 1, dtype=jnp.int32)
    owners = jnp.sum(jnp.where(slot_ids[None, :] == slot_range[:, None], entry_numbers[None, :], 0), axis=1) - 1
    return slot_ids, owners


def pack_rows(cotangent, moe_input, group_weight, expert_weight, expert_ids, experts_all, capacity):
    slot_ids, owners = slot_table(expert_ids, experts_all, capacity)
    present = owners >= 0
    entry_ids = jnp.maximum(owners, 0)
    token_ids = entry_ids // expert_ids.shape[1]
    route_weight = (group_weight[:, None] * expert_weight).reshape(-1)
    row_scale = jnp.where(present, route_weight[entry_ids], 0.0)
    cot_rows = (cotangent[token_ids].astype(jnp.float32) * row_scale[:, None]).astype(jnp.bfloat16)
    inp_rows = jnp.where(present[:, None], moe_input[token_ids], jnp.zeros((), moe_input.dtype))
    return cot_rows, inp_rows, slot_ids


def expert_grads(operands):
    rows_cot, rows_inp, w_gate, w_up, w_down = operands
    gate_pre = jnp.dot(rows_inp, w_gate, preferred_element_type=jnp.float32)
    up_pre = jnp.dot(rows_inp, w_up, preferred_element_type=jnp.float32)
    sigmoid_gate = jax.nn.sigmoid(gate_pre)
    hidden = (gate_pre * sigmoid_gate * up_pre).astype(jnp.bfloat16)
    grad_down = jnp.dot(hidden.T, rows_cot, preferred_element_type=jnp.float32).astype(jnp.bfloat16)
    hidden_grad = jnp.dot(rows_cot, w_down.T, preferred_element_type=jnp.float32)
    gate_grad = (hidden_grad * up_pre * sigmoid_gate * (1.0 + gate_pre * (1.0 - sigmoid_gate))).astype(jnp.bfloat16)
    up_grad = (hidden_grad * gate_pre * sigmoid_gate).astype(jnp.bfloat16)
    grad_gate = jnp.dot(rows_inp.T, gate_grad, preferred_element_type=jnp.float32).astype(jnp.bfloat16)
    grad_up = jnp.dot(rows_inp.T, up_grad, preferred_element_type=jnp.float32).astype(jnp.bfloat16)
    entry_sum = jnp.dot(gate_grad, w_gate.T, preferred_element_type=jnp.float32) + jnp.dot(up_grad, w_up.T, preferred_element_type=jnp.float32)
    entry_grad = entry_sum.astype(jnp.bfloat16)
    return grad_gate, grad_up, grad_down, entry_grad


def head_grads(operands):
    query_head, key_head, value_head, grad_head, rate_head = operands
    exact_result = lax.Precision.HIGHEST
    cumulative = jnp.cumsum(rate_head)
    mixing = jnp.exp(-jnp.abs(cumulative[:, None] - cumulative[None, :]))
    score_scale = KD ** -0.5
    scores = score_scale * jnp.dot(query_head.T, key_head, precision=exact_result) * mixing
    score_grad = score_scale * jnp.dot(grad_head.T, value_head, precision=exact_result) * mixing
    query_grad = jnp.dot(key_head, score_grad.T, precision=exact_result)
    key_grad = jnp.dot(query_head, score_grad, precision=exact_result)
    value_grad = jnp.dot(grad_head, scores, precision=exact_result)
    return query_grad, key_grad, value_grad


def reference(cotangent, moe_input, expert_ids, group_weight, expert_weight, mixer_out, queries, key_vectors, value_vectors, decay_rates, proj_weight, gate_weight, up_weight, down_weight):
    packer = jax.vmap(partial(pack_rows, experts_all=EXPERTS, capacity=CAP))
    cot_rows, inp_rows, slot_ids = packer(cotangent.reshape(N_SP, TOK_DEV, D), moe_input.reshape(N_SP, TOK_DEV, D), group_weight.reshape(N_SP, TOK_DEV), expert_weight.reshape(N_SP, TOK_DEV, TOP), expert_ids.reshape(N_SP, TOK_DEV, TOP))

    def by_expert(rows):
        return rows.reshape(N_SP, EXPERTS, CAP, D).transpose(1, 0, 2, 3).reshape(EXPERTS, N_SP * CAP, D)

    grad_gate, grad_up, grad_down, entry_grad = lax.map(expert_grads, (by_expert(cot_rows), by_expert(inp_rows), gate_weight, up_weight, down_weight))
    returned = entry_grad.reshape(EXPERTS, N_SP, CAP, D).transpose(1, 0, 2, 3).reshape(N_SP, EXPERTS * CAP, D)

    def pick_rows(rows, indices):
        return rows[indices]

    picked = jax.vmap(pick_rows)(returned, slot_ids)
    moe_grad = jnp.sum(picked.astype(jnp.float32).reshape(SEQUENCE_TOKENS, TOP, D), axis=1)
    resid_grad = (cotangent.astype(jnp.float32) + moe_grad).astype(jnp.bfloat16)
    grad_proj = jnp.dot(resid_grad.T, mixer_out, preferred_element_type=jnp.float32)
    out_grad = jnp.dot(proj_weight.T, resid_grad.T, preferred_element_type=jnp.float32)
    query_heads = queries.astype(jnp.float32).reshape(RETENTION_HEADS, KD, SEQUENCE_TOKENS)
    key_heads = key_vectors.astype(jnp.float32).reshape(RETENTION_HEADS, KD, SEQUENCE_TOKENS)
    value_heads = value_vectors.astype(jnp.float32).reshape(RETENTION_HEADS, VD, SEQUENCE_TOKENS)
    grad_heads = out_grad.reshape(RETENTION_HEADS, VD, SEQUENCE_TOKENS)
    query_grad, key_grad, value_grad = lax.map(head_grads, (query_heads, key_heads, value_heads, grad_heads, decay_rates))
    return (grad_gate, grad_up, grad_down, grad_proj, query_grad.reshape(RETENTION_HEADS * KD, SEQUENCE_TOKENS), key_grad.reshape(RETENTION_HEADS * KD, SEQUENCE_TOKENS), value_grad.reshape(RETENTION_HEADS * VD, SEQUENCE_TOKENS))
```

```python
import functools

import jax
import jax.numpy as jnp
from jax import lax
from jax.experimental import pallas as pl
from jax.experimental.pallas import tpu as pltpu
from jax.sharding import PartitionSpec as P

MESH = pl.DeviceIdType.MESH
VMEM = pl.BlockSpec(memory_space=pltpu.VMEM)


def near_first(count):
    order = [0]
    for step in range(1, count // 2 + 1):
        order.append(step)
        if count - step != step:
            order.append(count - step)
    return order


def greet(sp_count, tp_count, sp_place, tp_place, along_tp):
    barrier = pltpu.get_barrier_semaphore()
    for k in range(1, sp_count):
        pl.semaphore_signal(
            barrier,
            inc=1,
            device_id={"sp": lax.rem(sp_place + k, sp_count), "tp": tp_place},
            device_id_type=MESH,
        )
    if along_tp:
        for m in range(1, tp_count):
            pl.semaphore_signal(
                barrier,
                inc=1,
                device_id={"sp": sp_place, "tp": lax.rem(tp_place + m, tp_count)},
                device_id_type=MESH,
            )
    pl.semaphore_wait(barrier, sp_count - 1 + (tp_count - 1 if along_tp else 0))


def remote(src, dst, send_sem, recv_sem, sp_place, tp_place):
    return pltpu.make_async_remote_copy(
        src_ref=src,
        dst_ref=dst,
        send_sem=send_sem,
        recv_sem=recv_sem,
        device_id={"sp": sp_place, "tp": tp_place},
        device_id_type=MESH,
    )


def state_side(here, there, count):
    return (here + count - there) // count


def dispatch_kernel(
    sp_count, tp_count, cot_src, inp_src, state, cot_full, inp_full, state_all,
    local_sem, send_one, recv_one, send_two, recv_two, send_state, recv_state,
):
    me = lax.axis_index("sp")
    q = lax.axis_index("tp")
    width = cot_src.shape[2]
    square = tp_count == 4
    order = near_first(sp_count)
    arrays = ((cot_src, cot_full), (inp_src, inp_full))

    def columns(full, block, place):
        return full.at[block, :, pl.ds(pl.multiple_of(place * width, width), width)]

    if square:
        across_x = (q // 2) * 2 + (1 - lax.rem(q, 2))
        across_y = (1 - q // 2) * 2 + lax.rem(q, 2)
        across_both = (1 - q // 2) * 2 + (1 - lax.rem(q, 2))
        peers = (across_x, across_y)
        origins = (across_x, across_y)
    else:
        peers = tuple(lax.rem(q + m, tp_count) for m in range(1, tp_count))
        origins = tuple(lax.rem(q + tp_count - m, tp_count) for m in range(1, tp_count))

    greet(sp_count, tp_count, me, q, True)
    waits = []
    own = []
    for a, (src, full) in enumerate(arrays):
        copy = pltpu.make_async_copy(src.at[me], columns(full, me, q), local_sem.at[a])
        copy.start()
        own.append(copy)
    own_state = pltpu.make_async_copy(state.at[0], state_all.at[me], local_sem.at[2])
    own_state.start()
    for k in order[1:]:
        there = lax.rem(me + k, sp_count)
        for a, (src, full) in enumerate(arrays):
            copy = remote(
                src.at[there], columns(full, me, q), send_one.at[a, k], recv_one.at[a, k], there, q
            )
            copy.start()
            waits.append(copy)
    for k in order[1:]:
        there = lax.rem(me + k, sp_count)
        copy = remote(
            state.at[state_side(me, there, sp_count)],
            state_all.at[me],
            send_state.at[k],
            recv_state.at[k],
            there,
            q,
        )
        copy.start()
        waits.append(copy)

    def forward(k):
        block = lax.rem(me + sp_count - k, sp_count)
        for a, (src, full) in enumerate(arrays):
            if k == 0:
                own[a].wait()
            else:
                remote(
                    src.at[block], columns(full, block, q), send_one.at[a, k], recv_one.at[a, k], me, q
                ).wait_recv()
            for m, peer in enumerate(peers):
                piece = columns(full, block, q)
                copy = remote(piece, piece, send_two.at[a, k, m], recv_two.at[a, k, m], me, peer)
                copy.start()
                waits.append(copy)

    def arrived(a, k, m, place):
        block = lax.rem(me + sp_count - k, sp_count)
        piece = columns(arrays[a][1], block, place)
        remote(piece, piece, send_two.at[a, k, m], recv_two.at[a, k, m], me, q).wait_recv()
        return piece

    def relay(k):
        for a in range(2):
            for m, place in enumerate(origins):
                piece = arrived(a, k, m, place)
                if square and m == a:
                    copy = remote(
                        piece, piece, send_two.at[a, k, 2], recv_two.at[a, k, 2], me, peers[1 - a]
                    )
                    copy.start()
                    waits.append(copy)

    for number, k in enumerate(order):
        forward(k)
        if number:
            relay(order[number - 1])
    relay(order[-1])
    if square:
        for k in order:
            for a in range(2):
                arrived(a, k, 2, across_both)
    for k in order[1:]:
        source = lax.rem(me + sp_count - k, sp_count)
        remote(
            state.at[0], state_all.at[source], send_state.at[k], recv_state.at[k], me, q
        ).wait_recv()
    own_state.wait()
    for copy in waits:
        copy.wait_send()


def dispatch(cot_src, inp_src, state, sp_count, tp_count):
    rows, width = cot_src.shape[1:]
    full = jax.ShapeDtypeStruct((sp_count, rows, width * tp_count), cot_src.dtype)
    dma = pltpu.SemaphoreType.DMA
    return pl.pallas_call(
        functools.partial(dispatch_kernel, sp_count, tp_count),
        out_shape=(full, full, jax.ShapeDtypeStruct((sp_count,) + state.shape[1:], state.dtype)),
        in_specs=[VMEM] * 3,
        out_specs=(VMEM,) * 3,
        scratch_shapes=[
            dma((3,)),
            dma((2, sp_count)),
            dma((2, sp_count)),
            dma((2, sp_count, tp_count - 1)),
            dma((2, sp_count, tp_count - 1)),
            dma((sp_count,)),
            dma((sp_count,)),
        ],
        compiler_params=pltpu.CompilerParams(collective_id=0, has_side_effects=True),
    )(cot_src, inp_src, state)


def return_kernel(
    sp_count, tp_count, part, select, cot, resid,
    summed_in, outgoing, returned, send_rs, recv_rs, send_back, recv_back, send_ag, recv_ag,
):
    me = lax.axis_index("sp")
    q = lax.axis_index("tp")
    width = cot.shape[1]
    order = near_first(sp_count)

    def columns(place):
        return pl.ds(pl.multiple_of(place * width, width), width)

    greet(sp_count, tp_count, me, q, True)
    waits = []
    far_first = order[::-1]
    for k in far_first:
        block = lax.rem(me + k, sp_count)
        for m in range(1, tp_count):
            peer = lax.rem(q + m, tp_count)
            copy = remote(
                part.at[block, :, columns(peer)],
                summed_in.at[m - 1, block],
                send_rs.at[k, m - 1],
                recv_rs.at[k, m - 1],
                me,
                peer,
            )
            copy.start()
            waits.append(copy)
    for k in far_first:
        block = lax.rem(me + k, sp_count)
        total = part[block, :, columns(q)].astype(jnp.float32)
        for m in range(1, tp_count):
            remote(
                part.at[block, :, columns(q)],
                summed_in.at[m - 1, block],
                send_rs.at[k, m - 1],
                recv_rs.at[k, m - 1],
                me,
                q,
            ).wait_recv()
            total = total + summed_in[m - 1, block].astype(jnp.float32)
        outgoing[block] = total.astype(outgoing.dtype)
        if k:
            copy = remote(
                outgoing.at[block], returned.at[me], send_back.at[k], recv_back.at[k], block, q
            )
            copy.start()
            waits.append(copy)
    total = jnp.dot(select[me], outgoing[me], preferred_element_type=jnp.float32)
    for k in far_first[:-1]:
        source = lax.rem(me + sp_count - k, sp_count)
        remote(
            outgoing.at[source], returned.at[source], send_back.at[k], recv_back.at[k], me, q
        ).wait_recv()
        total = total + jnp.dot(
            select[source], returned[source], preferred_element_type=jnp.float32
        )
    resid[:, columns(q)] = (cot[...].astype(jnp.float32) + total).astype(resid.dtype)
    for m in range(1, tp_count):
        piece = resid.at[:, columns(q)]
        copy = remote(
            piece, piece, send_ag.at[m - 1], recv_ag.at[m - 1], me, lax.rem(q + m, tp_count)
        )
        copy.start()
        waits.append(copy)
    for m in range(1, tp_count):
        piece = resid.at[:, columns(lax.rem(q + tp_count - m, tp_count))]
        remote(piece, piece, send_ag.at[m - 1], recv_ag.at[m - 1], me, q).wait_recv()
    for copy in waits:
        copy.wait_send()


def bring_back(part, select, cot_slice, sp_count, tp_count):
    rows = part.shape[1]
    tokens, width = cot_slice.shape
    dma = pltpu.SemaphoreType.DMA
    return pl.pallas_call(
        functools.partial(return_kernel, sp_count, tp_count),
        out_shape=jax.ShapeDtypeStruct((tokens, width * tp_count), cot_slice.dtype),
        in_specs=[VMEM] * 3,
        out_specs=VMEM,
        scratch_shapes=[
            pltpu.VMEM((tp_count - 1, sp_count, rows, width), part.dtype),
            pltpu.VMEM((sp_count, rows, width), part.dtype),
            pltpu.VMEM((sp_count, rows, width), part.dtype),
            dma((sp_count, tp_count - 1)),
            dma((sp_count, tp_count - 1)),
            dma((sp_count,)),
            dma((sp_count,)),
            dma((tp_count - 1,)),
            dma((tp_count - 1,)),
        ],
        compiler_params=pltpu.CompilerParams(collective_id=1, has_side_effects=True),
    )(part, select, cot_slice)


def share_kernel(
    sp_count, tp_count, state, proj, state_all, proj_all,
    local_sem, send_state, recv_state, send_proj, recv_proj,
):
    me = lax.axis_index("sp")
    q = lax.axis_index("tp")
    order = near_first(sp_count)[1:][::-1]
    greet(sp_count, tp_count, me, q, False)
    own_state = pltpu.make_async_copy(state.at[0], state_all.at[me], local_sem.at[0])
    own_proj = pltpu.make_async_copy(proj.at[me], proj_all.at[me], local_sem.at[1])
    own_state.start()
    own_proj.start()
    waits = []
    for k in order:
        there = lax.rem(me + k, sp_count)
        side = state_side(me, there, sp_count)
        for copy in (
            remote(state.at[side], state_all.at[me], send_state.at[k], recv_state.at[k], there, q),
            remote(proj.at[there], proj_all.at[me], send_proj.at[k], recv_proj.at[k], there, q),
        ):
            copy.start()
            waits.append(copy)
    own_state.wait()
    own_proj.wait()
    for k in order:
        source = lax.rem(me + sp_count - k, sp_count)
        remote(
            state.at[0], state_all.at[source], send_state.at[k], recv_state.at[k], me, q
        ).wait_recv()
        remote(
            proj.at[source], proj_all.at[source], send_proj.at[k], recv_proj.at[k], me, q
        ).wait_recv()
    for copy in waits:
        copy.wait_send()


def share(state, proj, sp_count, tp_count):
    dma = pltpu.SemaphoreType.DMA
    return pl.pallas_call(
        functools.partial(share_kernel, sp_count, tp_count),
        out_shape=(
            jax.ShapeDtypeStruct((sp_count,) + state.shape[1:], state.dtype),
            jax.ShapeDtypeStruct(proj.shape, proj.dtype),
        ),
        in_specs=[VMEM] * 2,
        out_specs=(VMEM,) * 2,
        scratch_shapes=[
            dma((2,)), dma((sp_count,)), dma((sp_count,)), dma((sp_count,)), dma((sp_count,)),
        ],
        compiler_params=pltpu.CompilerParams(collective_id=2, has_side_effects=True),
    )(state, proj)


def slot_numbers(ids, experts_all, capacity):
    rows, top_count = ids.shape
    onehot = ids[:, :, None] == jnp.arange(experts_all, dtype=jnp.int32)
    row_tally = jnp.sum(onehot.astype(jnp.float32), axis=1)
    place = jnp.arange(rows, dtype=jnp.int32)
    below = (place[:, None] > place[None, :]).astype(jnp.bfloat16)
    before = jnp.dot(below, row_tally.astype(jnp.bfloat16), preferred_element_type=jnp.float32)
    slots = []
    for j in range(top_count):
        here = onehot[:, j].astype(jnp.float32)
        rank = jnp.sum(here * before, axis=1).astype(jnp.int32)
        before = before + here
        slots.append(ids[:, j] * capacity + rank)
    return slots


def expert_forward(cot_blocks, inp_blocks, gate_weight, up_weight, down_weight):
    gate_pre = jnp.einsum(
        "secd,edf->secf", inp_blocks, gate_weight, preferred_element_type=jnp.float32
    )
    up_pre = jnp.einsum("secd,edf->secf", inp_blocks, up_weight, preferred_element_type=jnp.float32)
    sigmoid_gate = jax.nn.sigmoid(gate_pre)
    hidden = (gate_pre * sigmoid_gate * up_pre).astype(jnp.bfloat16)
    hidden_grad = jnp.einsum(
        "secd,efd->secf", cot_blocks, down_weight, preferred_element_type=jnp.float32
    )
    gate_grad = (
        hidden_grad * up_pre * sigmoid_gate * (1.0 + gate_pre * (1.0 - sigmoid_gate))
    ).astype(jnp.bfloat16)
    up_grad = (hidden_grad * gate_pre * sigmoid_gate).astype(jnp.bfloat16)
    partial_grad = jnp.einsum(
        "secf,edf->secd", gate_grad, gate_weight, preferred_element_type=jnp.float32
    )
    partial_grad = partial_grad + jnp.einsum(
        "secf,edf->secd", up_grad, up_weight, preferred_element_type=jnp.float32
    )
    return hidden, gate_grad, up_grad, partial_grad.astype(jnp.bfloat16)


def on_device(
    cotangent,
    moe_input,
    expert_ids,
    group_weight,
    expert_weight,
    mixer_out,
    queries,
    key_vectors,
    value_vectors,
    decay_rates,
    proj_weight,
    gate_weight,
    up_weight,
    down_weight,
):
    exact = lax.Precision.HIGHEST
    sp_count = lax.axis_size("sp")
    tp_count = lax.axis_size("tp")
    me = lax.axis_index("sp")
    local_experts = gate_weight.shape[0]
    experts_all = local_experts * sp_count
    rows_here, model_width = cotangent.shape
    top_count = expert_ids.shape[1]
    capacity = 3 * top_count * rows_here // (2 * experts_all)
    slice_width = model_width // tp_count
    offset = lax.axis_index("tp") * slice_width
    slot_count = experts_all * capacity

    slots = slot_numbers(expert_ids, experts_all, capacity)
    slot_range = jnp.arange(slot_count, dtype=jnp.int32)
    hits = [slot_range[:, None] == s[None, :] for s in slots]
    select = functools.reduce(jnp.logical_or, hits).astype(jnp.bfloat16)
    route = group_weight[:, None] * expert_weight
    row_scale = sum(
        jnp.sum(jnp.where(h, route[:, j][None, :], 0.0), axis=1) for j, h in enumerate(hits)
    )
    cot_slice = lax.dynamic_slice_in_dim(cotangent, offset, slice_width, 1)
    inp_slice = lax.dynamic_slice_in_dim(moe_input, offset, slice_width, 1)
    cot_rows = jnp.dot(select, cot_slice, preferred_element_type=jnp.float32)
    cot_rows = (cot_rows * row_scale[:, None]).astype(jnp.bfloat16)
    inp_rows = jnp.dot(select, inp_slice, preferred_element_type=jnp.float32).astype(jnp.bfloat16)
    block_rows = local_experts * capacity

    heads_here, length = decay_rates.shape
    query_full = queries.astype(jnp.float32).reshape(heads_here, -1, length)
    key_full = key_vectors.astype(jnp.float32).reshape(heads_here, -1, length)
    value_full = value_vectors.astype(jnp.float32).reshape(heads_here, -1, length)
    key_size = query_full.shape[1]
    value_size = value_full.shape[1]
    score_scale = key_size ** (-0.5)
    place = jnp.arange(length, dtype=jnp.int32)
    prefix = jnp.dot(
        decay_rates, (place[:, None] <= place[None, :]).astype(jnp.float32), precision=exact
    )
    ending = prefix[:, -1:]
    mixing = score_scale * jnp.exp(-jnp.abs(prefix[:, :, None] - prefix[:, None, :]))
    toward_end = jnp.exp(prefix - ending)
    from_start = jnp.exp(-prefix)
    both_weights = jnp.stack([toward_end, from_start])
    key_state = jnp.einsum(
        "whkl,hvl->whkv", key_full[None] * both_weights[:, :, None, :], value_full, precision=exact
    )
    totals_rows = jnp.broadcast_to(
        ending[None, :, :, None], (2, heads_here, 8, value_size)
    )
    key_state = jnp.concatenate([key_state, totals_rows], axis=2)

    got_cot, got_inp, key_states = dispatch(
        cot_rows.reshape(sp_count, block_rows, slice_width),
        inp_rows.reshape(sp_count, block_rows, slice_width),
        key_state,
        sp_count,
        tp_count,
    )
    block_shape = (sp_count, local_experts, capacity, model_width)
    cot_blocks = got_cot.reshape(block_shape)
    inp_blocks = got_inp.reshape(block_shape)
    hidden, gate_grad, up_grad, partial_grad = expert_forward(
        cot_blocks, inp_blocks, gate_weight, up_weight, down_weight
    )

    select_back = select.reshape(sp_count, block_rows, rows_here).transpose(0, 2, 1)
    resid_grad = bring_back(
        partial_grad.reshape(sp_count, block_rows, model_width),
        select_back,
        cot_slice,
        sp_count,
        tp_count,
    )
    grad_down = jnp.einsum(
        "secf,secd->efd", hidden, cot_blocks, preferred_element_type=jnp.float32
    ).astype(jnp.bfloat16)
    grad_gate = jnp.einsum(
        "secd,secf->edf", inp_blocks, gate_grad, preferred_element_type=jnp.float32
    ).astype(jnp.bfloat16)
    grad_up = jnp.einsum(
        "secd,secf->edf", inp_blocks, up_grad, preferred_element_type=jnp.float32
    ).astype(jnp.bfloat16)

    proj_part = lax.dot_general(
        resid_grad, mixer_out, (((0,), (0,)), ((), ())), preferred_element_type=jnp.float32
    ).astype(jnp.bfloat16)
    out_grad = lax.dot_general(
        proj_weight, resid_grad, (((0,), (1,)), ((), ())), preferred_element_type=jnp.float32
    ).reshape(heads_here, -1, length)
    query_state = jnp.einsum(
        "whkl,hvl->whkv", query_full[None] * both_weights[:, :, None, :], out_grad, precision=exact
    )
    query_states, proj_parts = share(
        query_state, proj_part.reshape(sp_count, model_width // sp_count, -1), sp_count, tp_count
    )
    grad_proj = jnp.sum(proj_parts.astype(jnp.float32), axis=0)

    totals = key_states[:, :, key_size, 0]
    block = jnp.arange(sp_count, dtype=jnp.int32)
    low_between = (block[None, :] > block[:, None]) & (block[None, :] < me)
    high_between = (block[None, :] < block[:, None]) & (block[None, :] > me)
    low_decay = jnp.exp(-jnp.sum(jnp.where(low_between[:, :, None], totals[None], 0.0), axis=1))
    high_decay = jnp.exp(-jnp.sum(jnp.where(high_between[:, :, None], totals[None], 0.0), axis=1))
    low_decay = jnp.where((block < me)[:, None], low_decay, 0.0)
    high_decay = jnp.where((block > me)[:, None], high_decay, 0.0)
    both_decays = jnp.stack([low_decay, high_decay])[:, :, :, None, None]
    key_carried = jnp.sum(both_decays * key_states[None, :, :, :key_size], axis=1)
    query_carried = jnp.sum(both_decays * query_states[None], axis=1)

    scores = mixing * jnp.einsum("hkt,hks->hts", query_full, key_full, precision=exact)
    score_grad = mixing * jnp.einsum("hvt,hvs->hts", out_grad, value_full, precision=exact)
    query_grad = jnp.einsum("hks,hts->hkt", key_full, score_grad, precision=exact)
    key_grad = jnp.einsum("hkt,hts->hks", query_full, score_grad, precision=exact)
    value_grad = jnp.einsum("hvt,hts->hvs", out_grad, scores, precision=exact)
    reach = score_scale * jnp.stack([from_start, toward_end])
    out_reach = out_grad[None] * reach[:, :, None, :]
    value_reach = value_full[None] * reach[:, :, None, :]
    key_reach = key_full[None] * reach[:, :, None, :]
    query_grad = query_grad + jnp.einsum("whvl,whkv->hkl", out_reach, key_carried, precision=exact)
    key_grad = key_grad + jnp.einsum("whvl,whkv->hkl", value_reach, query_carried, precision=exact)
    value_grad = value_grad + jnp.einsum("whkl,whkv->hvl", key_reach, query_carried, precision=exact)
    return (
        grad_gate,
        grad_up,
        grad_down,
        grad_proj,
        query_grad.reshape(heads_here * key_size, length),
        key_grad.reshape(heads_here * key_size, length),
        value_grad.reshape(heads_here * value_size, length),
    )


def solution(mesh):
    return jax.shard_map(
        on_device,
        mesh=mesh,
        in_specs=(
            P("sp", None),
            P("sp", None),
            P("sp", None),
            P("sp"),
            P("sp", None),
            P("sp", "tp"),
            P("tp", "sp"),
            P("tp", "sp"),
            P("tp", "sp"),
            P("tp", "sp"),
            P(None, "tp"),
            P("sp", None, "tp"),
            P("sp", None, "tp"),
            P("sp", "tp", None),
        ),
        out_specs=(
            P("sp", None, "tp"),
            P("sp", None, "tp"),
            P("sp", "tp", None),
            P("sp", "tp"),
            P("tp", "sp"),
            P("tp", "sp"),
            P("tp", "sp"),
        ),
        check_vma=False,
    )
```

```python
import functools

import jax
import jax.numpy as jnp
from jax import lax
from jax.experimental import pallas as pl
from jax.experimental.pallas import tpu as pltpu
from jax.sharding import PartitionSpec as P

MESH = pl.DeviceIdType.MESH
VMEM = pl.BlockSpec(memory_space=pltpu.VMEM)


def near_first(count):
    order = [0]
    for step in range(1, count // 2 + 1):
        order.append(step)
        if count - step != step:
            order.append(count - step)
    return order


def greet_all(sp_count, tp_count, sp_place, tp_place, along_tp):
    barrier = pltpu.get_barrier_semaphore()
    for k in range(1, sp_count):
        pl.semaphore_signal(
            barrier,
            inc=1,
            device_id={"sp": lax.rem(sp_place + k, sp_count), "tp": tp_place},
            device_id_type=MESH,
        )
    if along_tp:
        for m in range(1, tp_count):
            pl.semaphore_signal(
                barrier,
                inc=1,
                device_id={"sp": sp_place, "tp": lax.rem(tp_place + m, tp_count)},
                device_id_type=MESH,
            )


def greet_wait(sp_count, tp_count, along_tp):
    barrier = pltpu.get_barrier_semaphore()
    pl.semaphore_wait(barrier, sp_count - 1 + (tp_count - 1 if along_tp else 0))


def greet(sp_count, tp_count, sp_place, tp_place, along_tp):
    greet_all(sp_count, tp_count, sp_place, tp_place, along_tp)
    greet_wait(sp_count, tp_count, along_tp)


def remote(src, dst, send_sem, recv_sem, sp_place, tp_place):
    return pltpu.make_async_remote_copy(
        src_ref=src,
        dst_ref=dst,
        send_sem=send_sem,
        recv_sem=recv_sem,
        device_id={"sp": sp_place, "tp": tp_place},
        device_id_type=MESH,
    )


def state_side(here, there, count):
    return (here + count - there) // count


def dispatch_kernel(
    sp_count, tp_count, capacity, ids, group, weight, cot, inp, keys, values, rates,
    cot_full, inp_full, state_all, select, cot_src, inp_src, state, local_sem, send_one, recv_one, send_two, recv_two, send_state, recv_state,
):
    me = lax.axis_index("sp")
    q = lax.axis_index("tp")
    width = cot_src.shape[2]
    square = tp_count == 4
    order = near_first(sp_count)
    arrays = ((cot_src, cot_full), (inp_src, inp_full))

    def columns(full, block, place):
        return full.at[block, :, pl.ds(pl.multiple_of(place * width, width), width)]

    if square:
        across_x = (q // 2) * 2 + (1 - lax.rem(q, 2))
        across_y = (1 - q // 2) * 2 + lax.rem(q, 2)
        across_both = (1 - q // 2) * 2 + (1 - lax.rem(q, 2))
        peers = (across_x, across_y)
        origins = (across_x, across_y)
    else:
        peers = tuple(lax.rem(q + m, tp_count) for m in range(1, tp_count))
        origins = tuple(lax.rem(q + tp_count - m, tp_count) for m in range(1, tp_count))

    greet_all(sp_count, tp_count, me, q, True)
    tokens, top_count = ids.shape
    block_rows = cot_src.shape[1]
    experts_all = sp_count * block_rows // capacity
    mine = pl.ds(pl.multiple_of(q * width, width), width)
    expert = lax.broadcasted_iota(jnp.int32, (tokens, experts_all), 1)
    named = [(ids[:, j : j + 1] == expert).astype(jnp.float32) for j in range(top_count)]
    below = lax.broadcasted_iota(jnp.int32, (tokens, tokens), 0) > lax.broadcasted_iota(
        jnp.int32, (tokens, tokens), 1
    )
    before = jnp.dot(
        below.astype(jnp.float32).astype(jnp.bfloat16),
        sum(named).astype(jnp.bfloat16),
        preferred_element_type=jnp.float32,
    )
    slots = []
    scaled = []
    cot_mine = cot[:, mine].astype(jnp.float32)
    inp_mine = inp[:, mine]
    for j in range(top_count):
        rank = jnp.sum(named[j] * before, axis=1, keepdims=True).astype(jnp.int32)
        before = before + named[j]
        slots.append(ids[:, j : j + 1] * capacity + rank)
        scaled.append((cot_mine * (group[...] * weight[:, j : j + 1])).astype(jnp.bfloat16))
    slot = lax.broadcasted_iota(jnp.int32, (tokens, block_rows), 1)

    def rows_of(picked, values):
        return lax.dot_general(
            picked, values, (((0,), (0,)), ((), ())), preferred_element_type=jnp.float32
        )

    def pack(k):
        there = lax.rem(me + k, sp_count)
        picks = [
            (s == slot + there * block_rows).astype(jnp.float32).astype(jnp.bfloat16)
            for s in slots
        ]
        cot_src[there] = sum(rows_of(p, v) for p, v in zip(picks, scaled)).astype(jnp.bfloat16)
        either = sum(picks)
        inp_src[there] = rows_of(either, inp_mine).astype(jnp.bfloat16)
        select[there] = either
        return there

    waits = []
    own = []
    pack(0)
    pack(order[1])
    greet_wait(sp_count, tp_count, True)
    for a, (src, full) in enumerate(arrays):
        copy = pltpu.make_async_copy(src.at[me], columns(full, me, q), local_sem.at[a])
        copy.start()
        own.append(copy)
    for k in order[1:]:
        there = lax.rem(me + k, sp_count)
        if k != order[1]:
            pack(k)
        for a, (src, full) in enumerate(arrays):
            copy = remote(
                src.at[there], columns(full, me, q), send_one.at[a, k], recv_one.at[a, k], there, q
            )
            copy.start()
            waits.append(copy)
    exact = lax.Precision.HIGHEST
    heads, length = rates.shape
    key_size = keys.shape[0] // heads
    value_size = values.shape[0] // heads
    upto = lax.broadcasted_iota(jnp.int32, (length, length), 0) <= lax.broadcasted_iota(
        jnp.int32, (length, length), 1
    )
    for h in range(heads):
        rate = jnp.broadcast_to(rates[h : h + 1, :], (8, length))
        prefix = jnp.dot(
            rate, upto.astype(jnp.float32), precision=exact, preferred_element_type=jnp.float32
        )[0:1]
        ending = prefix[:, length - 1 : length]
        key = keys[h * key_size : (h + 1) * key_size, :].astype(jnp.float32)
        value = values[h * value_size : (h + 1) * value_size, :].astype(jnp.float32)
        first = h * (key_size + 8)
        for side, reach in enumerate((jnp.exp(prefix - ending), jnp.exp(-prefix))):
            state[side, first : first + key_size, :] = lax.dot_general(
                key * reach,
                value,
                (((1,), (1,)), ((), ())),
                precision=exact,
                preferred_element_type=jnp.float32,
            )
            state[side, first + key_size : first + key_size + 8, :] = jnp.broadcast_to(
                ending, (8, value_size)
            )
    own_state = pltpu.make_async_copy(state.at[0], state_all.at[me], local_sem.at[2])
    own_state.start()
    for k in order[1:]:
        there = lax.rem(me + k, sp_count)
        copy = remote(
            state.at[state_side(me, there, sp_count)],
            state_all.at[me],
            send_state.at[k],
            recv_state.at[k],
            there,
            q,
        )
        copy.start()
        waits.append(copy)

    def forward(k):
        block = lax.rem(me + sp_count - k, sp_count)
        for a, (src, full) in enumerate(arrays):
            if k == 0:
                own[a].wait()
            else:
                remote(
                    src.at[block], columns(full, block, q), send_one.at[a, k], recv_one.at[a, k], me, q
                ).wait_recv()
            for m, peer in enumerate(peers):
                piece = columns(full, block, q)
                copy = remote(piece, piece, send_two.at[a, k, m], recv_two.at[a, k, m], me, peer)
                copy.start()
                waits.append(copy)

    def arrived(a, k, m, place):
        block = lax.rem(me + sp_count - k, sp_count)
        piece = columns(arrays[a][1], block, place)
        remote(piece, piece, send_two.at[a, k, m], recv_two.at[a, k, m], me, q).wait_recv()
        return piece

    def relay(k):
        for a in range(2):
            for m, place in enumerate(origins):
                piece = arrived(a, k, m, place)
                if square and m == a:
                    copy = remote(
                        piece, piece, send_two.at[a, k, 2], recv_two.at[a, k, 2], me, peers[1 - a]
                    )
                    copy.start()
                    waits.append(copy)

    for number, k in enumerate(order):
        forward(k)
        if number:
            relay(order[number - 1])
    relay(order[-1])
    if square:
        for k in order:
            for a in range(2):
                arrived(a, k, 2, across_both)
    for k in order[1:]:
        source = lax.rem(me + sp_count - k, sp_count)
        remote(
            state.at[0], state_all.at[source], send_state.at[k], recv_state.at[k], me, q
        ).wait_recv()
    own_state.wait()
    for copy in waits:
        copy.wait_send()


def dispatch(ids, group, weight, cot, inp, keys, values, rates, capacity, rows, sp_count, tp_count):
    tokens, model_width = cot.shape
    width = model_width // tp_count
    heads = rates.shape[0]
    state_rows = keys.shape[0] + 8 * heads
    value_size = values.shape[0] // heads
    full = jax.ShapeDtypeStruct((sp_count, rows, model_width), cot.dtype)
    dma = pltpu.SemaphoreType.DMA
    return pl.pallas_call(
        functools.partial(dispatch_kernel, sp_count, tp_count, capacity),
        out_shape=(
            full,
            full,
            jax.ShapeDtypeStruct((sp_count, state_rows, value_size), jnp.float32),
            jax.ShapeDtypeStruct((sp_count, tokens, rows), jnp.bfloat16),
        ),
        in_specs=[VMEM] * 8,
        out_specs=(VMEM,) * 4,
        scratch_shapes=[
            pltpu.VMEM((sp_count, rows, width), cot.dtype),
            pltpu.VMEM((sp_count, rows, width), inp.dtype),
            pltpu.VMEM((2, state_rows, value_size), jnp.float32),
            dma((3,)),
            dma((2, sp_count)),
            dma((2, sp_count)),
            dma((2, sp_count, tp_count - 1)),
            dma((2, sp_count, tp_count - 1)),
            dma((sp_count,)),
            dma((sp_count,)),
        ],
        compiler_params=pltpu.CompilerParams(collective_id=0, has_side_effects=True),
    )(ids, group, weight, cot, inp, keys, values, rates)


def return_kernel(
    sp_count, tp_count, part, select, cot, resid,
    summed_in, outgoing, returned, send_rs, recv_rs, send_back, recv_back, send_ag, recv_ag,
):
    me = lax.axis_index("sp")
    q = lax.axis_index("tp")
    width = cot.shape[1] // tp_count
    order = near_first(sp_count)

    def columns(place):
        return pl.ds(pl.multiple_of(place * width, width), width)

    greet(sp_count, tp_count, me, q, True)
    waits = []
    far_first = order[::-1]
    for k in far_first:
        block = lax.rem(me + k, sp_count)
        for m in range(1, tp_count):
            peer = lax.rem(q + m, tp_count)
            copy = remote(
                part.at[block, :, columns(peer)],
                summed_in.at[m - 1, block],
                send_rs.at[k, m - 1],
                recv_rs.at[k, m - 1],
                me,
                peer,
            )
            copy.start()
            waits.append(copy)
    for k in far_first:
        block = lax.rem(me + k, sp_count)
        total = part[block, :, columns(q)].astype(jnp.float32)
        for m in range(1, tp_count):
            remote(
                part.at[block, :, columns(q)],
                summed_in.at[m - 1, block],
                send_rs.at[k, m - 1],
                recv_rs.at[k, m - 1],
                me,
                q,
            ).wait_recv()
            total = total + summed_in[m - 1, block].astype(jnp.float32)
        outgoing[block] = total.astype(outgoing.dtype)
        if k:
            copy = remote(
                outgoing.at[block], returned.at[me], send_back.at[k], recv_back.at[k], block, q
            )
            copy.start()
            waits.append(copy)
    total = jnp.dot(select[me], outgoing[me], preferred_element_type=jnp.float32)
    for k in far_first[:-1]:
        source = lax.rem(me + sp_count - k, sp_count)
        remote(
            outgoing.at[source], returned.at[source], send_back.at[k], recv_back.at[k], me, q
        ).wait_recv()
        total = total + jnp.dot(
            select[source], returned[source], preferred_element_type=jnp.float32
        )
    resid[:, columns(q)] = (cot[:, columns(q)].astype(jnp.float32) + total).astype(resid.dtype)
    for m in range(1, tp_count):
        piece = resid.at[:, columns(q)]
        copy = remote(
            piece, piece, send_ag.at[m - 1], recv_ag.at[m - 1], me, lax.rem(q + m, tp_count)
        )
        copy.start()
        waits.append(copy)
    for m in range(1, tp_count):
        piece = resid.at[:, columns(lax.rem(q + tp_count - m, tp_count))]
        remote(piece, piece, send_ag.at[m - 1], recv_ag.at[m - 1], me, q).wait_recv()
    for copy in waits:
        copy.wait_send()


def bring_back(part, select, cot, sp_count, tp_count):
    rows = part.shape[1]
    width = cot.shape[1] // tp_count
    dma = pltpu.SemaphoreType.DMA
    return pl.pallas_call(
        functools.partial(return_kernel, sp_count, tp_count),
        out_shape=jax.ShapeDtypeStruct(cot.shape, cot.dtype),
        in_specs=[VMEM] * 3,
        out_specs=VMEM,
        scratch_shapes=[
            pltpu.VMEM((tp_count - 1, sp_count, rows, width), part.dtype),
            pltpu.VMEM((sp_count, rows, width), part.dtype),
            pltpu.VMEM((sp_count, rows, width), part.dtype),
            dma((sp_count, tp_count - 1)),
            dma((sp_count, tp_count - 1)),
            dma((sp_count,)),
            dma((sp_count,)),
            dma((tp_count - 1,)),
            dma((tp_count - 1,)),
        ],
        compiler_params=pltpu.CompilerParams(collective_id=1, has_side_effects=True),
    )(part, select, cot)


def expert_forward(cot_blocks, inp_blocks, gate_weight, up_weight, down_weight):
    gate_pre = jnp.einsum(
        "secd,edf->secf", inp_blocks, gate_weight, preferred_element_type=jnp.float32
    )
    up_pre = jnp.einsum("secd,edf->secf", inp_blocks, up_weight, preferred_element_type=jnp.float32)
    sigmoid_gate = jax.nn.sigmoid(gate_pre)
    hidden = (gate_pre * sigmoid_gate * up_pre).astype(jnp.bfloat16)
    hidden_grad = jnp.einsum(
        "secd,efd->secf", cot_blocks, down_weight, preferred_element_type=jnp.float32
    )
    gate_grad = (
        hidden_grad * up_pre * sigmoid_gate * (1.0 + gate_pre * (1.0 - sigmoid_gate))
    ).astype(jnp.bfloat16)
    up_grad = (hidden_grad * gate_pre * sigmoid_gate).astype(jnp.bfloat16)
    partial_grad = jnp.einsum(
        "secf,edf->secd", gate_grad, gate_weight, preferred_element_type=jnp.float32
    )
    partial_grad = partial_grad + jnp.einsum(
        "secf,edf->secd", up_grad, up_weight, preferred_element_type=jnp.float32
    )
    return hidden, gate_grad, up_grad, partial_grad.astype(jnp.bfloat16)


def on_device(
    cotangent,
    moe_input,
    expert_ids,
    group_weight,
    expert_weight,
    mixer_out,
    queries,
    key_vectors,
    value_vectors,
    decay_rates,
    proj_weight,
    gate_weight,
    up_weight,
    down_weight,
):
    exact = lax.Precision.HIGHEST
    sp_count = lax.axis_size("sp")
    tp_count = lax.axis_size("tp")
    me = lax.axis_index("sp")
    local_experts = gate_weight.shape[0]
    experts_all = local_experts * sp_count
    rows_here, model_width = cotangent.shape
    top_count = expert_ids.shape[1]
    capacity = 3 * top_count * rows_here // (2 * experts_all)
    block_rows = local_experts * capacity

    heads_here, length = decay_rates.shape
    query_full = queries.astype(jnp.float32).reshape(heads_here, -1, length)
    key_full = key_vectors.astype(jnp.float32).reshape(heads_here, -1, length)
    value_full = value_vectors.astype(jnp.float32).reshape(heads_here, -1, length)
    key_size = query_full.shape[1]
    value_size = value_full.shape[1]
    score_scale = key_size ** (-0.5)
    place = jnp.arange(length, dtype=jnp.int32)
    prefix = jnp.dot(
        decay_rates, (place[:, None] <= place[None, :]).astype(jnp.float32), precision=exact
    )
    ending = prefix[:, -1:]
    mixing = score_scale * jnp.exp(-jnp.abs(prefix[:, :, None] - prefix[:, None, :]))
    toward_end = jnp.exp(prefix - ending)
    from_start = jnp.exp(-prefix)
    both_weights = jnp.stack([toward_end, from_start])
    got_cot, got_inp, key_states, select = dispatch(
        expert_ids,
        group_weight[:, None],
        expert_weight,
        cotangent,
        moe_input,
        key_vectors,
        value_vectors,
        decay_rates,
        capacity,
        block_rows,
        sp_count,
        tp_count,
    )
    key_states = key_states.reshape(sp_count, heads_here, -1, value_size)
    block_shape = (sp_count, local_experts, capacity, model_width)
    cot_blocks = got_cot.reshape(block_shape)
    inp_blocks = got_inp.reshape(block_shape)
    hidden, gate_grad, up_grad, partial_grad = expert_forward(
        cot_blocks, inp_blocks, gate_weight, up_weight, down_weight
    )

    resid_grad = bring_back(
        partial_grad.reshape(sp_count, block_rows, model_width), select, cotangent, sp_count, tp_count
    )
    grad_down = jnp.einsum(
        "secf,secd->efd", hidden, cot_blocks, preferred_element_type=jnp.float32
    ).astype(jnp.bfloat16)
    grad_gate = jnp.einsum(
        "secd,secf->edf", inp_blocks, gate_grad, preferred_element_type=jnp.float32
    ).astype(jnp.bfloat16)
    grad_up = jnp.einsum(
        "secd,secf->edf", inp_blocks, up_grad, preferred_element_type=jnp.float32
    ).astype(jnp.bfloat16)

    proj_part = lax.dot_general(
        resid_grad, mixer_out, (((0,), (0,)), ((), ())), preferred_element_type=jnp.float32
    ).astype(jnp.bfloat16)
    out_grad = lax.dot_general(
        proj_weight, resid_grad, (((0,), (1,)), ((), ())), preferred_element_type=jnp.float32
    ).reshape(heads_here, -1, length)
    query_state = jnp.einsum(
        "whkl,hvl->whkv", query_full[None] * both_weights[:, :, None, :], out_grad, precision=exact
    )
    block = jnp.arange(sp_count, dtype=jnp.int32)
    query_state = query_state.astype(jnp.bfloat16).transpose(0, 2, 1, 3)
    query_state = query_state.reshape(2, key_size, heads_here * value_size)
    sent = jnp.concatenate(
        [
            proj_part.reshape(sp_count, -1, heads_here * value_size),
            jnp.where((block > me)[:, None, None], query_state[:1], query_state[1:]),
        ],
        axis=1,
    )
    shared = lax.all_to_all(sent, "sp", split_axis=0, concat_axis=0, tiled=True)
    shared = shared.astype(jnp.float32)
    proj_rows = model_width // sp_count
    grad_proj = jnp.sum(shared[:, :proj_rows], axis=0)
    query_states = shared[:, proj_rows:].reshape(sp_count, key_size, heads_here, value_size)
    query_states = query_states.transpose(0, 2, 1, 3)

    totals = key_states[:, :, key_size, 0]
    low_between = (block[None, :] > block[:, None]) & (block[None, :] < me)
    high_between = (block[None, :] < block[:, None]) & (block[None, :] > me)
    low_decay = jnp.exp(-jnp.sum(jnp.where(low_between[:, :, None], totals[None], 0.0), axis=1))
    high_decay = jnp.exp(-jnp.sum(jnp.where(high_between[:, :, None], totals[None], 0.0), axis=1))
    low_decay = jnp.where((block < me)[:, None], low_decay, 0.0)
    high_decay = jnp.where((block > me)[:, None], high_decay, 0.0)
    both_decays = jnp.stack([low_decay, high_decay])[:, :, :, None, None]
    key_carried = jnp.sum(both_decays * key_states[None, :, :, :key_size], axis=1)
    query_carried = jnp.sum(both_decays * query_states[None], axis=1)

    scores = mixing * jnp.einsum("hkt,hks->hts", query_full, key_full, precision=exact)
    score_grad = mixing * jnp.einsum("hvt,hvs->hts", out_grad, value_full, precision=exact)
    query_grad = jnp.einsum("hks,hts->hkt", key_full, score_grad, precision=exact)
    key_grad = jnp.einsum("hkt,hts->hks", query_full, score_grad, precision=exact)
    value_grad = jnp.einsum("hvt,hts->hvs", out_grad, scores, precision=exact)
    reach = score_scale * jnp.stack([from_start, toward_end])
    out_reach = out_grad[None] * reach[:, :, None, :]
    value_reach = value_full[None] * reach[:, :, None, :]
    key_reach = key_full[None] * reach[:, :, None, :]
    query_grad = query_grad + jnp.einsum("whvl,whkv->hkl", out_reach, key_carried, precision=exact)
    key_grad = key_grad + jnp.einsum("whvl,whkv->hkl", value_reach, query_carried, precision=exact)
    value_grad = value_grad + jnp.einsum("whkl,whkv->hvl", key_reach, query_carried, precision=exact)
    return (
        grad_gate,
        grad_up,
        grad_down,
        grad_proj,
        query_grad.reshape(heads_here * key_size, length),
        key_grad.reshape(heads_here * key_size, length),
        value_grad.reshape(heads_here * value_size, length),
    )


def solution(mesh):
    return jax.shard_map(
        on_device,
        mesh=mesh,
        in_specs=(
            P("sp", None),
            P("sp", None),
            P("sp", None),
            P("sp"),
            P("sp", None),
            P("sp", "tp"),
            P("tp", "sp"),
            P("tp", "sp"),
            P("tp", "sp"),
            P("tp", "sp"),
            P(None, "tp"),
            P("sp", None, "tp"),
            P("sp", None, "tp"),
            P("sp", "tp", None),
        ),
        out_specs=(
            P("sp", None, "tp"),
            P("sp", None, "tp"),
            P("sp", "tp", None),
            P("sp", "tp"),
            P("tp", "sp"),
            P("tp", "sp"),
            P("tp", "sp"),
        ),
        check_vma=False,
    )
```
